256 devices in a mesh: sp: 32 (over z, x), tp: 8 (over y, core).
Axes of the slice: x: 4, y: 4, z: 8, core: 2. Of those that a mesh axis runs over, the one named last changes fastest.
Arguments:
- tokens: bfloat16 [24576, 4096], P('sp', 'tp'), may hold values from -6 to 6
- norm_gain: float32 [4096], replicated, may hold values from 0.1 to 1.9
- w_query: bfloat16 [4096, 2048], P('sp', 'tp'), may hold values from -0.09375 to 0.09375
- w_key: bfloat16 [4096, 1024], P('sp', 'tp'), may hold values from -0.09375 to 0.09375
- w_value: bfloat16 [4096, 1024], P('sp', 'tp'), may hold values from -0.09375 to 0.09375
- w_pool: bfloat16 [4096, 1024], P('sp', 'tp'), may hold values from -0.09375 to 0.09375
- query_gain: float32 [64], replicated, may hold values from 0.5 to 8
- key_gain: float32 [64], replicated, may hold values from 0.5 to 8
- sink_logit: float32 [32], P('tp'), may hold values from 1 to 5
- w_out_pool: bfloat16 [1024, 4096], P('tp', 'sp'), may hold values from -0.75 to 0.75
- w_out_attn: bfloat16 [2048, 4096], P('tp', 'sp'), may hold values from -1.5 to 1.5
Outputs:
- mixed: bfloat16 [24576, 4096], P(('sp', 'tp'))
The draws below stay inside these ranges and needn't reach their ends.
All inputs are finite; a program needn't handle non-finite values.
Results may differ from the reference program's by a relative error of at most 0.014.
The reference program's roundings to bfloat16 on the way count: a program that leaves them out, or rounds other values in their place, can miss the bound.
Values may be sent and summed in bfloat16 or wider, within the bound.
No kernel may reach another device: no remote copies, remote signals or barrier semaphores. Data moves between devices by JAX's collectives and lax.ppermute only.
A program may use at most 128 MiB of HBM per device.

```python
import jax
import jax.numpy as jnp
from jax import lax

D = 4096
HEADS = 32
KV_HEADS = 16
HEAD = 64
POOL = 1024
WINDOW = 128
GRID_W = 64
SEQ = 24576
N_TP = 8


def draw_query_gain(key, part):
    return jax.random.uniform(jax.random.fold_in(key, 11), (HEAD,), jnp.float32, 0.5, 1.5)


def draw_key_gain(key, part):
    return jax.random.uniform(jax.random.fold_in(key, 23), (HEAD,), jnp.float32, 0.5, 1.5)


def shard_levels(key, extent, cuts, smallest, high):
    level = 1.0
    for dim, blocks in cuts:
        steps = jax.random.uniform(jax.random.fold_in(jax.random.fold_in(key, 6), dim), (blocks,), jnp.float32, smallest / len(cuts), high / len(cuts))
        level = level * jnp.repeat(jnp.exp(steps), extent[dim] // blocks).reshape((-1,) + (1,) * (len(extent) - 1 - dim))
    return level


def scatter_about(key, shape, spread, most, shards=(), kind=jnp.bfloat16):
    array = spread * jax.random.normal(key, shape, jnp.float32)
    if shards:
        array = array * shard_levels(key, shape, shards, -0.22, 0.18)
    return jnp.clip(array, -most, most).astype(kind)


def setup_inputs(seed: int = 0) -> dict:
    keys = jax.random.split(jax.random.key(seed), 12)
    return {
        "tokens": scatter_about(keys[0], (SEQ, D), 1.0, 6.0, ((0, 32), (1, 8))),
        "norm_gain": jnp.clip(1.0 + 0.18 * jax.random.normal(keys[1], (D,), jnp.float32), 0.1, 1.9),
        "w_query": scatter_about(keys[2], (D, HEADS * HEAD), D ** -0.5, 0.09375, ((0, 32), (1, 8))),
        "w_key": scatter_about(keys[3], (D, KV_HEADS * HEAD), D ** -0.5, 0.09375, ((0, 32), (1, 8))),
        "w_value": scatter_about(keys[4], (D, KV_HEADS * HEAD), D ** -0.5, 0.09375, ((0, 32), (1, 8))),
        "w_pool": scatter_about(keys[5], (D, POOL), D ** -0.5, 0.09375, ((0, 32), (1, 8))),
        "query_gain": draw_query_gain(jax.random.fold_in(keys[11], 71), 0),
        "key_gain": draw_key_gain(jax.random.fold_in(keys[11], 71), 0),
        "sink_logit": jnp.clip(1.0 + 4.0 * jax.random.uniform(keys[8], (HEADS,), jnp.float32) ** shard_levels(keys[8], (HEADS,), ((0, 8),), -0.2, 0.2), 1.0, 5.0),
        "w_out_pool": scatter_about(keys[9], (POOL, D), (POOL // 16) ** -0.5, 0.75, ((0, 8), (1, 32))),
        "w_out_attn": scatter_about(keys[10], (HEADS * HEAD, D), (HEADS * HEAD // 128) ** -0.5, 1.5, ((0, 8), (1, 32))),
    }


eps = 1e-06
rope_base = 10000.0
neg_big = -1e+30

def rope_tables(positions, head_size):
    quarter = head_size // 4
    freqs = 1.0 / rope_base ** (jnp.arange(quarter, dtype=jnp.float32) * 2.0 / (head_size // 2))
    row_angle = (positions // GRID_W).astype(jnp.float32)[:, None] * freqs
    col_angle = (positions % GRID_W).astype(jnp.float32)[:, None] * freqs
    angles = jnp.concatenate([row_angle, row_angle, col_angle, col_angle], axis=-1)
    return (jnp.cos(angles), jnp.sin(angles))

def rotate(heads_in, cosine, sine):
    part_one, part_two, part_three, part_four = jnp.split(heads_in, 4, axis=-1)
    turned = jnp.concatenate([-part_two, part_one, -part_four, part_three], axis=-1)
    return heads_in * cosine[:, None, :] + turned * sine[:, None, :]

def prepare(projected, gain, cosine, sine):
    rows_count = projected.shape[0]
    shaped = projected.reshape(rows_count, -1, HEAD)
    scaled = shaped * lax.rsqrt(lax.optimization_barrier(jnp.mean(shaped * shaped, axis=-1, keepdims=True)) + eps) * gain
    return rotate(scaled, cosine, sine).reshape(rows_count, -1).astype(jnp.bfloat16)

def reference(tokens, norm_gain, w_query, w_key, w_value, w_pool, query_gain, key_gain, sink_logit, w_out_pool, w_out_attn):
    seq = tokens.shape[0]
    widened = tokens.astype(jnp.float32)
    normed = (widened * lax.rsqrt(lax.optimization_barrier(jnp.mean(widened * widened, axis=1, keepdims=True)) + eps) * norm_gain).astype(jnp.bfloat16)
    query_raw = jnp.dot(normed, w_query, preferred_element_type=jnp.float32)
    key_raw = jnp.dot(normed, w_key, preferred_element_type=jnp.float32)
    values_all = jnp.dot(normed, w_value, preferred_element_type=jnp.float32).astype(jnp.bfloat16)
    pool_in = jnp.dot(normed, w_pool, preferred_element_type=jnp.float32).astype(jnp.bfloat16)
    positions = jnp.arange(seq, dtype=jnp.int32)
    cosine, sine = rope_tables(positions, HEAD)
    queries = prepare(query_raw, query_gain, cosine, sine)
    keys_all = prepare(key_raw, key_gain, cosine, sine)
    group = HEADS // KV_HEADS
    blocks = seq // WINDOW
    padded_keys = jnp.pad(keys_all, ((WINDOW, WINDOW), (0, 0)))
    padded_values = jnp.pad(values_all, ((WINDOW, WINDOW), (0, 0)))
    sink = sink_logit.astype(jnp.float32).reshape(KV_HEADS, group, 1, 1)

    def one_block(index):
        first_row = index * WINDOW
        block_q = lax.dynamic_slice_in_dim(queries, first_row, WINDOW, 0).reshape(WINDOW, KV_HEADS, group, HEAD).astype(jnp.float32)
        block_k = lax.dynamic_slice_in_dim(padded_keys, first_row, 3 * WINDOW, 0).reshape(3 * WINDOW, KV_HEADS, HEAD).astype(jnp.float32)
        block_v = lax.dynamic_slice_in_dim(padded_values, first_row, 3 * WINDOW, 0).reshape(3 * WINDOW, KV_HEADS, HEAD).astype(jnp.float32)
        scores = jnp.einsum('qhgd,khd->hgqk', block_q, block_k) * HEAD ** (-0.5)
        query_pos = first_row + jnp.arange(WINDOW, dtype=jnp.int32)[:, None]
        key_pos = first_row - WINDOW + jnp.arange(3 * WINDOW, dtype=jnp.int32)[None, :]
        inside = (jnp.abs(query_pos - key_pos) <= WINDOW) & (key_pos >= 0) & (key_pos < seq)
        scores = jnp.where(inside, scores, neg_big)
        top = jnp.maximum(lax.optimization_barrier(jnp.max(scores, axis=-1, keepdims=True)), sink)
        raised = jnp.exp(scores - top)
        totals = lax.optimization_barrier(jnp.sum(raised, axis=-1, keepdims=True)) + jnp.exp(sink - top)
        weights = (raised / totals).astype(jnp.bfloat16)
        result = jnp.einsum('hgqk,khd->qhgd', weights.astype(jnp.float32), block_v)
        return result.reshape(WINDOW, HEADS * HEAD).astype(jnp.bfloat16)
    attended = lax.map(one_block, jnp.arange(blocks, dtype=jnp.int32)).reshape(seq, HEADS * HEAD)
    pool_wide = pool_in.astype(jnp.float32)
    prefix = jnp.concatenate([jnp.zeros((1, POOL), jnp.float32), jnp.cumsum(pool_wide, axis=0)], axis=0)
    group_ch = POOL // 4
    levels = []
    for level in range(4):
        reach = 2 ** level
        low = jnp.clip(positions - reach, 0, seq - 1)
        high = jnp.clip(positions + reach - 1, 0, seq - 1)
        counted = (high - low + 1).astype(jnp.float32)
        columns = prefix[:, level * group_ch:(level + 1) * group_ch]
        summed = columns[high + 1] - columns[low]
        levels.append(summed / counted[:, None])
    pooled = jnp.concatenate(levels, axis=1).astype(jnp.bfloat16)
    pool_cols = POOL // N_TP
    attn_cols = HEADS * HEAD // N_TP
    outcome = jnp.zeros((seq, D), jnp.float32)
    for block_index in range(N_TP):
        term = jnp.dot(pooled[:, block_index * pool_cols:(block_index + 1) * pool_cols], w_out_pool[block_index * pool_cols:(block_index + 1) * pool_cols], preferred_element_type=jnp.float32)
        term = term + jnp.dot(attended[:, block_index * attn_cols:(block_index + 1) * attn_cols], w_out_attn[block_index * attn_cols:(block_index + 1) * attn_cols], preferred_element_type=jnp.float32)
        outcome = outcome + lax.optimization_barrier(term.astype(jnp.bfloat16)).astype(jnp.float32)
    return outcome.astype(jnp.bfloat16)
```

```python
import jax
import jax.numpy as jnp
import numpy as np
from jax import lax
from jax.experimental import pallas as pl
from jax.experimental.pallas import tpu as pltpu
from jax.sharding import PartitionSpec as P

HEAD = 64
WINDOW = 128
GRID_W = 64
NX, NZ, NY = 4, 8, 4
TILE = 128
LANES = 128
ROWS = 256

eps = 1e-06
rope_base = 10000.0
neg_big = -1e30
pool_reach = 8


Y_ORDER = (0, -1, 1, 2)
X_ORDER = (0, -1, 1, 2)
Z_ORDER = (0, -1, 1, -2, 2, -3, 3, 4)


def spot():
    sp, tp = lax.axis_index("sp"), lax.axis_index("tp")
    return lax.div(sp, NX), lax.rem(sp, NX), lax.div(tp, 2), lax.rem(tp, 2)


def around(place, offset, count):
    return lax.rem(place + (offset + count), count)


def z_moves(step):
    return [(z * NX + x, (z + step) % NZ * NX + x) for z in range(NZ) for x in range(NX)]


def x_moves(step):
    return [(z * NX + x, z * NX + (x + step) % NX) for z in range(NZ) for x in range(NX)]


def y_moves(step):
    return [(y * 2 + c, (y + step) % NY * 2 + c) for y in range(NY) for c in range(2)]


core_moves = [(t, t ^ 1) for t in range(2 * NY)]
split_moves = [
    (2 * y + c, (y + 1 - 2 * c) % NY * 2 + c) for y in range(NY) for c in range(2)
]


def cost(flops, nbytes):
    return pl.CostEstimate(flops=flops, bytes_accessed=nbytes, transcendentals=0)


def whole_spec(a):
    return pl.BlockSpec(a.shape, lambda i: (0,) * a.ndim)


vmem = pl.BlockSpec(memory_space=pltpu.VMEM)
smem = pl.BlockSpec(memory_space=pltpu.SMEM)


def tile_body(wq, wk, wv, wp, wop, woa, first, second):
    first[0] = wq[:, :LANES]
    first[1] = wq[:, LANES:]
    first[2] = wop[...]
    first[3] = woa[:TILE]
    first[4] = woa[TILE:]
    second[0] = wk[...]
    second[1] = wv[...]
    second[2] = wp[...]


def tile_call(*weights):
    return pl.pallas_call(
        tile_body,
        out_shape=(
            jax.ShapeDtypeStruct((5, TILE, LANES), jnp.bfloat16),
            jax.ShapeDtypeStruct((3, TILE, LANES), jnp.bfloat16),
        ),
        in_specs=[vmem] * 6,
        out_specs=(vmem, vmem),
        name="tiles",
        cost_estimate=cost(1000000, 500000),
    )(*weights)


def norm_body(*refs):
    pieces, gain, out = refs[:8], refs[8], refs[9]
    _, _, y, core = spot()
    places = [2 * around(y, step, NY) + c for c in (core, 1 - core) for step in Y_ORDER]

    def chunk(i, carry):
        here = pl.ds(pl.multiple_of(i * 16, 16), 16)
        total = None
        for piece in pieces:
            wide = piece[here].astype(jnp.float32)
            square = wide * wide
            for k in range(0, square.shape[1], LANES):
                part = square[:, k : k + LANES]
                total = part if total is None else total + part
        scale = lax.rsqrt(jnp.sum(total, axis=1, keepdims=True) / (8.0 * 512.0) + eps)
        for piece, place in zip(pieces, places):
            wide = piece[here].astype(jnp.float32)
            out[place, here] = (wide * scale * gain[place]).astype(jnp.bfloat16)
        return carry

    lax.fori_loop(0, TILE // 16, chunk, 0, unroll=2)


def norm_call(pieces, gain):
    rows, width = pieces[0].shape
    return pl.pallas_call(
        norm_body,
        out_shape=jax.ShapeDtypeStruct((8, rows, width), jnp.bfloat16),
        grid=(rows // TILE,),
        in_specs=[pl.BlockSpec((TILE, width), lambda i: (i, 0))] * 8
        + [pl.BlockSpec((8, 1, width), lambda i: (0, 0, 0))],
        out_specs=pl.BlockSpec((8, TILE, width), lambda i: (0, i, 0)),
        cost_estimate=cost(40 * rows * 8 * width, 4 * rows * 8 * width),
        name="norm",
    )(*pieces, gain)


def turn_tables(first_row, size):
    within = np.arange(LANES) % HEAD
    freqs = (1.0 / np.float32(rope_base) ** (np.arange(16, dtype=np.float32) * np.float32(2.0 / 32))).astype(np.float32)
    freq = jnp.asarray(freqs[within % 16])[None]
    row_lane = jnp.asarray(within < 32)[None]
    sign = jnp.asarray(np.where(within % 32 < 16, -1.0, 1.0).astype(np.float32))[None]
    at = jnp.arange(size, dtype=jnp.int32)[:, None]
    place = jnp.where(at < GRID_W, at, first_row + at - GRID_W).astype(jnp.float32)
    angle = place * freq
    mine = (at >= GRID_W) == row_lane
    return jnp.stack([jnp.where(mine, jnp.cos(angle), 0.0), jnp.where(mine, jnp.sin(angle) * sign, 0.0)])


def headed(part, gain, cosine, sine):
    lane = lax.broadcasted_iota(jnp.int32, part.shape, 1)
    left = lane < HEAD
    square = part * part
    low = jnp.sum(jnp.where(left, square, 0.0), axis=1, keepdims=True)
    high = jnp.sum(jnp.where(left, 0.0, square), axis=1, keepdims=True)
    scale = jnp.where(left, lax.rsqrt(low / HEAD + eps), lax.rsqrt(high / HEAD + eps))
    scaled = part * scale * gain
    turned = jnp.where(
        lane % 32 < 16, pltpu.roll(scaled, LANES - 16, 1), pltpu.roll(scaled, 16, 1)
    )
    return (scaled * cosine + turned * sine).astype(jnp.bfloat16)


def project_body(xn, *refs):
    by_z, by_x = refs[:8], refs[8:12]
    q_gain, k_gain, turns, q_out, kvp_out, weights = refs[12:]
    step = pl.program_id(0)

    @pl.when(step == 0)
    def _():
        z, x, _, _ = spot()
        z_at = [around(z, offset, NZ) for offset in Z_ORDER]
        x_at = [around(x, offset, NX) for offset in X_ORDER]
        for i in range(8):
            for j in range(4):
                here = pl.ds(pl.multiple_of(x_at[j] * TILE, TILE), TILE)
                for k in range(2):
                    weights[z_at[i], here, k * LANES : (k + 1) * LANES] = by_x[j][i, k]
                for k in range(3):
                    weights[z_at[i], here, (2 + k) * LANES : (3 + k) * LANES] = by_z[i][j, k]

    total = None
    for k in range(8):
        part = jnp.dot(xn[k], weights[k], preferred_element_type=jnp.float32)
        total = part if total is None else total + part
    for g in range(ROWS // GRID_W):
        here = slice(g * GRID_W, (g + 1) * GRID_W)
        row = GRID_W + step * (ROWS // GRID_W) + g
        cosine = turns[0, :GRID_W] + turns[0, pl.ds(row, 1)]
        sine = turns[1, :GRID_W] + turns[1, pl.ds(row, 1)]
        for j in range(3):
            made = headed(
                total[here, j * LANES : (j + 1) * LANES],
                q_gain[...] if j < 2 else k_gain[...],
                cosine,
                sine,
            )
            if j < 2:
                q_out[here, j * LANES : (j + 1) * LANES] = made
            else:
                kvp_out[here, :LANES] = made
    kvp_out[:, LANES:] = total[:, 3 * LANES :].astype(jnp.bfloat16)


def project_call(xn, by_z, by_x, q_gain, k_gain, turns):
    rows = xn.shape[1]
    return pl.pallas_call(
        project_body,
        out_shape=(
            jax.ShapeDtypeStruct((rows, 256), jnp.bfloat16),
            jax.ShapeDtypeStruct((rows, 384), jnp.bfloat16),
        ),
        grid=(rows // ROWS,),
        in_specs=[pl.BlockSpec((8, ROWS, 512), lambda i: (0, i, 0))]
        + [whole_spec(a) for a in (*by_z, *by_x, q_gain, k_gain, turns)],
        out_specs=(
            pl.BlockSpec((ROWS, 256), lambda i: (i, 0)),
            pl.BlockSpec((ROWS, 384), lambda i: (i, 0)),
        ),
        scratch_shapes=[pltpu.VMEM((8, 512, 640), jnp.bfloat16)],
        cost_estimate=cost(2 * rows * 4096 * 640, 2 * rows * 4096 + 2 * 4096 * 640),
        name="project",
    )(xn, *by_z, *by_x, q_gain, k_gain, turns)


def attention_body(
    sink, q, kvp, low, high, out, keys, values, queries, scores, probs, scales, band
):
    rows = q.shape[0]
    blocks = rows // WINDOW
    _, _, level, _ = spot()
    start = lax.axis_index("sp") * rows
    seq = NZ * NX * rows
    span = 3 * WINDOW

    for part, first, size in ((low, 0, WINDOW), (kvp, WINDOW, rows), (high, WINDOW + rows, WINDOW)):
        for half, held in ((0, keys), (1, values)):
            block = part[:, half * LANES : (half + 1) * LANES]
            held[0, first : first + size] = block
            held[1, first : first + size] = jnp.concatenate(
                [block[:, HEAD:], block[:, :HEAD]], axis=1
            )
    left = lax.broadcasted_iota(jnp.int32, (rows, LANES), 1) < HEAD
    for j in range(2):
        pair = q[:, j * LANES : (j + 1) * LANES] * HEAD ** (-0.5)
        for e in range(2):
            alone = jnp.where(left if e == 0 else ~left, pair, 0).astype(jnp.bfloat16)
            for b in range(blocks):
                queries[int(e != j), b, j * WINDOW : (j + 1) * WINDOW] = alone[
                    b * WINDOW : (b + 1) * WINDOW
                ]

    pool_low = low[WINDOW - 16 :, 2 * LANES :].astype(jnp.float32)[16 - pool_reach :]
    pool_high = high[:16, 2 * LANES :].astype(jnp.float32)[:pool_reach]
    band[:pool_reach] = jnp.where(start > 0, pool_low, 0.0)
    band[pool_reach : pool_reach + rows] = kvp[:, 2 * LANES :].astype(jnp.float32)
    band[pool_reach + rows :] = jnp.where(start + rows < seq, pool_high, 0.0)
    position = start + lax.broadcasted_iota(jnp.int32, (rows, LANES), 0)
    for side in range(4):
        reach = 2**side

        @pl.when(level == side)
        def _():
            total = band[pool_reach - reach : pool_reach + reach + rows - 1]
            for k in range(side + 1):
                width = 2**k
                total = total[:-width] + total[width:]
            first = jnp.maximum(position - reach, 0)
            last = jnp.minimum(position + reach - 1, seq - 1)
            counted = (last - first + 1).astype(jnp.float32)
            out[:, :LANES] = (total / counted).astype(jnp.bfloat16)

    for b in range(blocks):
        for kind in range(2):
            scores[b, kind] = lax.dot_general(
                queries[kind, b],
                keys[kind, b * WINDOW : b * WINDOW + span],
                (((1,), (1,)), ((), ())),
                preferred_element_type=jnp.float32,
            )

    ahead = lax.broadcasted_iota(jnp.int32, (WINDOW, span), 1) - lax.broadcasted_iota(
        jnp.int32, (WINDOW, span), 0
    )
    near = (ahead >= 0) & (ahead <= 2 * WINDOW)
    key_at = lax.broadcasted_iota(jnp.int32, (WINDOW, span), 1)

    def soften(b, carry):
        origin = start + (b - 1) * WINDOW
        inside = near & (key_at >= -origin) & (key_at < seq - origin)
        for kind in range(2):
            for j in range(2):
                logit = sink[2 * j + (j if kind == 0 else 1 - j)]
                here = pl.ds(j * WINDOW, WINDOW)
                score = jnp.where(inside, scores[b, kind, here], neg_big)
                top = jnp.maximum(jnp.max(score, axis=1, keepdims=True), logit)
                raised = jnp.exp(score - top)
                totals = jnp.sum(raised, axis=1, keepdims=True) + jnp.exp(logit - top)
                probs[b, kind, here] = raised.astype(jnp.bfloat16)
                scales[b, kind, here] = jnp.broadcast_to(1.0 / totals, (WINDOW, LANES))
        return carry

    lax.fori_loop(0, blocks, soften, 0)

    half = lax.broadcasted_iota(jnp.int32, (WINDOW, LANES), 1) < HEAD
    for b in range(blocks):
        made = [
            jnp.dot(
                probs[b, kind],
                values[kind, b * WINDOW : b * WINDOW + span],
                preferred_element_type=jnp.float32,
            )
            * scales[b, kind]
            for kind in range(2)
        ]
        for j in range(2):
            parts = [m[j * WINDOW : (j + 1) * WINDOW] for m in made]
            both = jnp.where(half, parts[j], parts[1 - j])
            out[b * WINDOW : (b + 1) * WINDOW, (1 + j) * LANES : (2 + j) * LANES] = both.astype(
                jnp.bfloat16
            )


def attention_call(sink, q, kvp, low, high):
    rows = q.shape[0]
    blocks = rows // WINDOW
    return pl.pallas_call(
        attention_body,
        out_shape=jax.ShapeDtypeStruct((rows, 384), jnp.bfloat16),
        in_specs=[smem] + [vmem] * 4,
        out_specs=vmem,
        scratch_shapes=[
            pltpu.VMEM((2, rows + 2 * WINDOW, LANES), jnp.bfloat16),
            pltpu.VMEM((2, rows + 2 * WINDOW, LANES), jnp.bfloat16),
            pltpu.VMEM((2, blocks, 2 * WINDOW, LANES), jnp.bfloat16),
            pltpu.VMEM((blocks, 2, 2 * WINDOW, 3 * WINDOW), jnp.float32),
            pltpu.VMEM((blocks, 2, 2 * WINDOW, 3 * WINDOW), jnp.bfloat16),
            pltpu.VMEM((blocks, 2, 2 * WINDOW, LANES), jnp.float32),
            pltpu.VMEM((rows + 2 * pool_reach, LANES), jnp.float32),
        ],
        cost_estimate=cost(60 * rows * 4 * 3 * WINDOW * 4, 4 * rows * 256 * 2),
        name="attention",
    )(sink, q, kvp, low, high)


def order_body(*refs):
    by_x, out = refs[:4], refs[4]
    z, x, _, _ = spot()
    for i, offset in enumerate(Z_ORDER):
        z_at = around(z, offset, NZ)
        for j, step in enumerate(X_ORDER):
            here = pl.ds(pl.multiple_of(around(x, step, NX) * LANES, LANES), LANES)
            for k in range(3):
                out[z_at, k * TILE : (k + 1) * TILE, here] = by_x[j][i, k]


def order_call(by_x):
    return pl.pallas_call(
        order_body,
        out_shape=jax.ShapeDtypeStruct((8, 3 * TILE, 4 * LANES), jnp.bfloat16),
        in_specs=[vmem] * 4,
        out_specs=vmem,
        cost_estimate=cost(5000000, 6000000),
        name="order",
    )(*by_x)


def out_body(att, weights, mine, theirs, done):
    total = jnp.dot(att[...], weights[...], preferred_element_type=jnp.float32)
    done[...] = total.astype(jnp.bfloat16).reshape(done.shape)
    _, _, y, core = spot()
    for r in range(4):
        owner = 2 * around(y, r, NY)
        mine[r] = done[owner + core]
        theirs[r] = done[owner + 1 - core]


def out_call(att, weights, part, parts):
    rows = att.shape[0]
    share = rows // 8
    columns = 4 * LANES
    steps = 8 // parts
    made = jax.ShapeDtypeStruct((4, share, steps * columns), jnp.bfloat16)
    spec = pl.BlockSpec((4, share, columns), lambda i: (0, 0, i))
    return pl.pallas_call(
        out_body,
        out_shape=(made, made),
        grid=(steps,),
        in_specs=[
            whole_spec(att),
            pl.BlockSpec((None, 3 * TILE, columns), lambda i: (i + part * steps, 0, 0)),
        ],
        out_specs=(spec, spec),
        scratch_shapes=[pltpu.VMEM((8, share, columns), jnp.bfloat16)],
        cost_estimate=cost(2 * rows * 384 * 512 * steps, 2 * rows * 512 * steps),
    )(att, weights)


def ring_z(own, far):
    up, down = own, own
    held = [own]
    for _ in range(1, 4):
        up = lax.ppermute(up, "sp", z_moves(1))
        down = lax.ppermute(down, "sp", z_moves(-1))
        held += [up, down]
    return held + [lax.ppermute(up if far == 1 else down, "sp", z_moves(far))]


def ring_x(own, far):
    before = lax.ppermute(own, "sp", x_moves(1))
    after = lax.ppermute(own, "sp", x_moves(-1))
    return [own, before, after, lax.ppermute(before if far == 1 else after, "sp", x_moves(far))]


def plus(*parts):
    total = parts[0].astype(jnp.float32)
    for part in parts[1:]:
        total = total + part.astype(jnp.float32)
    return total.astype(jnp.bfloat16)


def scatter_sum(mine, theirs):
    swapped = lax.ppermute(theirs, "tp", core_moves)
    half = mine.shape[1] // 2
    low = lax.ppermute(plus(mine[2, :half], swapped[2, :half]), "tp", y_moves(1))
    high = lax.ppermute(plus(mine[2, half:], swapped[2, half:]), "tp", y_moves(-1))
    up = jnp.concatenate(
        [plus(mine[1, :half], swapped[1, :half], low), plus(mine[1, half:], swapped[1, half:])]
    )
    down = jnp.concatenate(
        [plus(mine[3, :half], swapped[3, :half]), plus(mine[3, half:], swapped[3, half:], high)]
    )
    return plus(
        mine[0],
        swapped[0],
        lax.ppermute(up, "tp", y_moves(1)),
        lax.ppermute(down, "tp", y_moves(-1)),
    )


def layer(
    tokens,
    norm_gain,
    w_query,
    w_key,
    w_value,
    w_pool,
    query_gain,
    key_gain,
    sink_logit,
    w_out_pool,
    w_out_attn,
):
    rows = tokens.shape[0]
    sp, tp = lax.axis_index("sp"), lax.axis_index("tp")

    before = lax.ppermute(tokens, "tp", y_moves(1))
    after = lax.ppermute(tokens, "tp", y_moves(-1))
    w_block, kvp_block = tile_call(w_query, w_key, w_value, w_pool, w_out_pool, w_out_attn)

    near = [lax.ppermute(kvp_block, "sp", x_moves(-step)) for i, step in enumerate(X_ORDER) if i]
    held = ring_z(w_block, 1)
    by_z = ring_z(jnp.stack([kvp_block] + near), -1)
    farthest = lax.ppermute(jnp.where(tp % 2 == 0, before, after), "tp", split_moves)
    pieces = [tokens, before, after, farthest]
    pieces += [lax.ppermute(a, "tp", core_moves) for a in pieces]
    by_x = ring_x(jnp.stack([a[:2] for a in held]), 1)
    out_by_x = ring_x(jnp.stack([a[2:] for a in held]), -1)

    turns = turn_tables(sp * (rows // GRID_W), 80)
    twice = lambda g: jnp.concatenate([g, g]).reshape(1, LANES)

    xn = norm_call(pieces, norm_gain.reshape(8, 1, -1))
    q, kvp = project_call(xn, by_z, by_x, twice(query_gain), twice(key_gain), turns)
    count = NZ * NX
    forward = [(i, (i + 1) % count) for i in range(count)]
    backward = [(b, a) for a, b in forward]
    low = lax.ppermute(kvp[-WINDOW:], "sp", forward)
    high = lax.ppermute(kvp[:WINDOW], "sp", backward)
    weights = order_call(out_by_x)
    att = attention_call(sink_logit, q, kvp, low, high)
    sums = [scatter_sum(*out_call(att, weights, part, 2)) for part in range(2)]
    return jnp.concatenate([s.reshape(rows // 8, -1) for s in sums], axis=1)


def solution(mesh):
    placed = (
        P("sp", "tp"),
        P(),
        P("sp", "tp"),
        P("sp", "tp"),
        P("sp", "tp"),
        P("sp", "tp"),
        P(),
        P(),
        P("tp"),
        P("tp", "sp"),
        P("tp", "sp"),
    )
    return jax.shard_map(
        layer, mesh=mesh, in_specs=placed, out_specs=P(("sp", "tp"), None), check_vma=False
    )
```

```python
import functools

import jax
import jax.numpy as jnp
import numpy as np
from jax import lax
from jax.experimental import pallas as pl
from jax.experimental.pallas import tpu as pltpu
from jax.sharding import PartitionSpec as P

HEAD = 64
WINDOW = 128
GRID_W = 64
NX, NZ, NY = 4, 8, 4
TILE = 128
LANES = 128
ROWS = 256

eps = 1e-06
rope_base = 10000.0
neg_big = -1e30
pool_reach = 8


Y_ORDER = (0, -1, 1, 2)
X_ORDER = (0, -1, 1, 2)
Z_ORDER = (0, -1, 1, -2, 2, -3, 3, 4)


def spot():
    sp, tp = lax.axis_index("sp"), lax.axis_index("tp")
    return lax.div(sp, NX), lax.rem(sp, NX), lax.div(tp, 2), lax.rem(tp, 2)


def around(place, offset, count):
    return lax.rem(place + (offset + count), count)


def z_moves(step):
    return [(z * NX + x, (z + step) % NZ * NX + x) for z in range(NZ) for x in range(NX)]


def x_moves(step):
    return [(z * NX + x, z * NX + (x + step) % NX) for z in range(NZ) for x in range(NX)]


def y_moves(step):
    return [(y * 2 + c, (y + step) % NY * 2 + c) for y in range(NY) for c in range(2)]


core_moves = [(t, t ^ 1) for t in range(2 * NY)]
split_moves = [
    (2 * y + c, (y + 1 - 2 * c) % NY * 2 + c) for y in range(NY) for c in range(2)
]


def cost(flops, nbytes):
    return pl.CostEstimate(flops=flops, bytes_accessed=nbytes, transcendentals=0)


def limit(mebibytes):
    return pltpu.CompilerParams(vmem_limit_bytes=mebibytes << 20)


def zigzag(i):
    return lax.select(lax.rem(i, 2) == 1, -lax.div(i + 1, 2), lax.div(i, 2))


vmem = pl.BlockSpec(memory_space=pltpu.VMEM)
smem = pl.BlockSpec(memory_space=pltpu.SMEM)


def tile_body(wq, wk, wv, wp, wop, woa, first, second):
    first[0] = wq[:, :LANES]
    first[1] = wq[:, LANES:]
    first[2] = wop[...]
    first[3] = woa[:TILE]
    first[4] = woa[TILE:]
    second[0] = wk[...]
    second[1] = wv[...]
    second[2] = wp[...]


def tile_call(*weights):
    return pl.pallas_call(
        tile_body,
        out_shape=(
            jax.ShapeDtypeStruct((5, TILE, LANES), jnp.bfloat16),
            jax.ShapeDtypeStruct((3, TILE, LANES), jnp.bfloat16),
        ),
        in_specs=[vmem] * 6,
        out_specs=(vmem, vmem),
        name="tiles",
        cost_estimate=cost(1000000, 500000),
    )(*weights)


def regroup_body(*refs):
    blocks, first, second = refs[:8], refs[8], refs[9]
    for i, block in enumerate(blocks):
        first[i] = block[:2]
        second[i] = block[2:]


def regroup_call(blocks):
    return pl.pallas_call(
        regroup_body,
        out_shape=(
            jax.ShapeDtypeStruct((8, 2, TILE, LANES), jnp.bfloat16),
            jax.ShapeDtypeStruct((8, 3, TILE, LANES), jnp.bfloat16),
        ),
        in_specs=[vmem] * 8,
        out_specs=(vmem, vmem),
        name="regroup",
        cost_estimate=cost(2000000, 2600000),
    )(*blocks)


def token_places(y, core):
    return [2 * around(y, step, NY) + core for step in Y_ORDER]


def square_body(*refs):
    pieces, squares = refs[:4], refs[4]

    def chunk(i, carry):
        here = pl.ds(pl.multiple_of(i * 16, 16), 16)
        total = None
        for piece in pieces:
            wide = piece[here].astype(jnp.float32)
            square = wide * wide
            for k in range(0, square.shape[1], LANES):
                part = square[:, k : k + LANES]
                total = part if total is None else total + part
        squares[here] = total
        return carry

    lax.fori_loop(0, squares.shape[0] // 16, chunk, 0, unroll=2)


def square_call(pieces):
    rows, width = pieces[0].shape
    return pl.pallas_call(
        square_body,
        out_shape=jax.ShapeDtypeStruct((rows, LANES), jnp.float32),
        in_specs=[vmem] * 4,
        out_specs=vmem,
        cost_estimate=cost(10 * rows * 4 * width, 2 * rows * 4 * width),
        name="square",
        compiler_params=limit(6),
    )(*pieces)


def norm_body(*refs):
    pieces, gain, own_squares, other_squares, out = refs[:4], *refs[4:]
    _, _, y, core = spot()
    gains = [gain[place] for place in token_places(y, core)]

    def chunk(i, carry):
        here = pl.ds(pl.multiple_of(i * 32, 32), 32)
        square = jnp.sum(own_squares[here] + other_squares[here], axis=1, keepdims=True)
        scale = lax.rsqrt(square / (8.0 * 512.0) + eps)
        for p, piece in enumerate(pieces):
            wide = piece[here].astype(jnp.float32)
            out[p, here] = (wide * scale * gains[p]).astype(jnp.bfloat16)
        return carry

    lax.fori_loop(0, out.shape[1] // 32, chunk, 0, unroll=2)


def norm_call(pieces, gain, squares):
    rows, width = pieces[0].shape
    return pl.pallas_call(
        norm_body,
        out_shape=jax.ShapeDtypeStruct((4, rows, width), jnp.bfloat16),
        in_specs=[vmem] * 7,
        out_specs=vmem,
        cost_estimate=cost(20 * rows * 4 * width, 2 * rows * 8 * width),
        name="norm",
        compiler_params=limit(10),
    )(*pieces, gain, *squares)


def turn_tables(first_row, size):
    within = np.arange(LANES) % HEAD
    freqs = (1.0 / np.float32(rope_base) ** (np.arange(16, dtype=np.float32) * np.float32(2.0 / 32))).astype(np.float32)
    freq = jnp.asarray(freqs[within % 16])[None]
    row_lane = jnp.asarray(within < 32)[None]
    sign = jnp.asarray(np.where(within % 32 < 16, -1.0, 1.0).astype(np.float32))[None]
    at = jnp.arange(size, dtype=jnp.int32)[:, None]
    place = jnp.where(at < GRID_W, at, first_row + at - GRID_W).astype(jnp.float32)
    angle = place * freq
    mine = (at >= GRID_W) == row_lane
    return jnp.stack([jnp.where(mine, jnp.cos(angle), 0.0), jnp.where(mine, jnp.sin(angle) * sign, 0.0)])


def headed(part, gain, cosine, sine):
    lane = lax.broadcasted_iota(jnp.int32, part.shape, 1)
    left = lane < HEAD
    square = part * part
    low = jnp.sum(jnp.where(left, square, 0.0), axis=1, keepdims=True)
    high = jnp.sum(jnp.where(left, 0.0, square), axis=1, keepdims=True)
    scale = jnp.where(left, lax.rsqrt(low / HEAD + eps), lax.rsqrt(high / HEAD + eps))
    scaled = part * scale * gain
    turned = jnp.where(
        lane % 32 < 16, pltpu.roll(scaled, LANES - 16, 1), pltpu.roll(scaled, 16, 1)
    )
    return (scaled * cosine + turned * sine).astype(jnp.bfloat16)


def multiply(own_x, other_x, weights, total):
    _, _, y, core = spot()
    pieces = [
        (part, p, place)
        for part, c in ((own_x, core), (other_x, 1 - core))
        for p, place in enumerate(token_places(y, c))
    ]

    def over_blocks(step, carry):
        block = pl.ds(pl.multiple_of(step * ROWS, ROWS), ROWS)
        made = None
        for part, p, place in pieces:
            one = jnp.dot(part[p, block], weights[place], preferred_element_type=jnp.float32)
            made = one if made is None else made + one
        total[block] = made
        return carry

    lax.fori_loop(0, total.shape[0] // ROWS, over_blocks, 0)


SPAN = 2 * GRID_W


def turned_rows(turns, g):
    rows = [pl.ds(GRID_W + g * (SPAN // GRID_W) + i, 1) for i in range(SPAN // GRID_W)]
    return [
        jnp.concatenate([turns[t, :GRID_W] + turns[t, row] for row in rows], axis=0)
        for t in range(2)
    ]


def kvp_body(own_x, other_x, *refs):
    by_z = refs[:8]
    gain, turns, out, first_out, last_out, weights, total = refs[8:]
    z, x, _, _ = spot()
    z_at = [around(z, offset, NZ) for offset in Z_ORDER]
    rows = out.shape[0]

    def over_x(j, carry):
        here = pl.ds(pl.multiple_of(around(x, zigzag(j), NX) * TILE, TILE), TILE)
        for i in range(8):
            for k in range(3):
                weights[z_at[i], here, k * LANES : (k + 1) * LANES] = by_z[i][j, k]
        return carry

    lax.fori_loop(0, 4, over_x, 0)
    multiply(own_x, other_x, weights, total)

    def over_rows(g, carry):
        here = pl.ds(pl.multiple_of(g * SPAN, SPAN), SPAN)
        cosine, sine = turned_rows(turns, g)
        out[here, :LANES] = headed(total[here, :LANES], gain[...], cosine, sine)
        out[here, LANES:] = total[here, LANES:].astype(jnp.bfloat16)
        return carry

    lax.fori_loop(0, rows // SPAN, over_rows, 0)
    first_out[...] = out[:WINDOW]
    last_out[...] = out[rows - WINDOW :]


def q_body(own_x, other_x, *refs):
    by_x = refs[:4]
    gain, turns, out, weights, total = refs[4:]
    z, x, _, _ = spot()
    x_at = [around(x, offset, NX) for offset in X_ORDER]

    def over_z(i, carry):
        to = around(z, zigzag(i), NZ)
        for j in range(4):
            here = pl.ds(pl.multiple_of(x_at[j] * TILE, TILE), TILE)
            for k in range(2):
                weights[to, here, k * LANES : (k + 1) * LANES] = by_x[j][i, k]
        return carry

    lax.fori_loop(0, 8, over_z, 0)
    multiply(own_x, other_x, weights, total)

    def over_rows(g, carry):
        here = pl.ds(pl.multiple_of(g * SPAN, SPAN), SPAN)
        cosine, sine = turned_rows(turns, g)
        for j in range(2):
            lanes = slice(j * LANES, (j + 1) * LANES)
            out[here, lanes] = headed(total[here, lanes], gain[...], cosine, sine)
        return carry

    lax.fori_loop(0, out.shape[0] // SPAN, over_rows, 0)


def kvp_call(xs, by_z, gain, turns):
    rows = xs[0].shape[1]
    edge = jax.ShapeDtypeStruct((WINDOW, 384), jnp.bfloat16)
    return pl.pallas_call(
        kvp_body,
        out_shape=(jax.ShapeDtypeStruct((rows, 384), jnp.bfloat16), edge, edge),
        in_specs=[vmem] * 12,
        out_specs=(vmem,) * 3,
        scratch_shapes=[
            pltpu.VMEM((8, 512, 384), jnp.bfloat16),
            pltpu.VMEM((rows, 384), jnp.float32),
        ],
        cost_estimate=cost(2 * rows * 4096 * 384, 2 * rows * 4096 + 2 * 4096 * 384),
        name="kvp",
        compiler_params=limit(18),
    )(*xs, *by_z, gain, turns)


def q_call(xs, by_x, gain, turns):
    rows = xs[0].shape[1]
    return pl.pallas_call(
        q_body,
        out_shape=jax.ShapeDtypeStruct((rows, 256), jnp.bfloat16),
        in_specs=[vmem] * 8,
        out_specs=vmem,
        scratch_shapes=[
            pltpu.VMEM((8, 512, 256), jnp.bfloat16),
            pltpu.VMEM((rows, 256), jnp.float32),
        ],
        cost_estimate=cost(2 * rows * 4096 * 256, 2 * rows * 4096 + 2 * 4096 * 256),
        name="q",
        compiler_params=limit(16),
    )(*xs, *by_x, gain, turns)


def attention_body(
    sink, q, kvp, low, high, out, keys, values, queries, scores, probs, scales, band
):
    rows = q.shape[0]
    blocks = rows // WINDOW
    _, _, level, _ = spot()
    start = lax.axis_index("sp") * rows
    seq = NZ * NX * rows
    span = 3 * WINDOW

    for part, first, size in ((low, 0, WINDOW), (kvp, WINDOW, rows), (high, WINDOW + rows, WINDOW)):
        for half, held in ((0, keys), (1, values)):
            block = part[:, half * LANES : (half + 1) * LANES]
            held[0, first : first + size] = block
            held[1, first : first + size] = jnp.concatenate(
                [block[:, HEAD:], block[:, :HEAD]], axis=1
            )
    left = lax.broadcasted_iota(jnp.int32, (rows, LANES), 1) < HEAD
    for j in range(2):
        pair = q[:, j * LANES : (j + 1) * LANES] * HEAD ** (-0.5)
        for e in range(2):
            alone = jnp.where(left if e == 0 else ~left, pair, 0).astype(jnp.bfloat16)
            queries[int(e != j), :, j * WINDOW : (j + 1) * WINDOW] = alone.reshape(
                blocks, WINDOW, LANES
            )

    pool_low = low[WINDOW - 16 :, 2 * LANES :].astype(jnp.float32)[16 - pool_reach :]
    pool_high = high[:16, 2 * LANES :].astype(jnp.float32)[:pool_reach]
    band[:pool_reach] = jnp.where(start > 0, pool_low, 0.0)
    band[pool_reach : pool_reach + rows] = kvp[:, 2 * LANES :].astype(jnp.float32)
    band[pool_reach + rows :] = jnp.where(start + rows < seq, pool_high, 0.0)
    at = lax.broadcasted_iota(jnp.int32, (WINDOW, LANES), 0)
    reach = lax.shift_left(jnp.int32(1), level)

    def pool(b, carry):
        total = band[pl.ds(pl.multiple_of(b * WINDOW, WINDOW), WINDOW + 2 * pool_reach)]
        chosen = None
        for side in range(4):
            width = 2**side
            total = total[:-width] + total[width:]
            part = total[pool_reach - width : pool_reach - width + WINDOW]
            chosen = part if chosen is None else jnp.where(level == side, part, chosen)
        position = start + b * WINDOW + at
        first = jnp.maximum(position - reach, 0)
        last = jnp.minimum(position + reach - 1, seq - 1)
        counted = (last - first + 1).astype(jnp.float32)
        here = pl.ds(pl.multiple_of(b * WINDOW, WINDOW), WINDOW)
        out[here, :LANES] = (chosen / counted).astype(jnp.bfloat16)
        return carry

    lax.fori_loop(0, blocks, pool, 0)

    def score(b, carry):
        there = pl.ds(pl.multiple_of(b * WINDOW, WINDOW), span)
        for kind in range(2):
            scores[b, kind] = lax.dot_general(
                queries[kind, b],
                keys[kind, there],
                (((1,), (1,)), ((), ())),
                preferred_element_type=jnp.float32,
            )
        return carry

    lax.fori_loop(0, blocks, score, 0, unroll=2)

    ahead = lax.broadcasted_iota(jnp.int32, (WINDOW, span), 1) - lax.broadcasted_iota(
        jnp.int32, (WINDOW, span), 0
    )
    near = (ahead >= 0) & (ahead <= 2 * WINDOW)
    key_at = lax.broadcasted_iota(jnp.int32, (WINDOW, span), 1)

    def soften(b, carry):
        origin = start + (b - 1) * WINDOW
        inside = near & (key_at >= -origin) & (key_at < seq - origin)
        for kind in range(2):
            for j in range(2):
                logit = sink[2 * j + (j if kind == 0 else 1 - j)]
                here = pl.ds(j * WINDOW, WINDOW)
                score = jnp.where(inside, scores[b, kind, here], neg_big)
                top = jnp.maximum(jnp.max(score, axis=1, keepdims=True), logit)
                raised = jnp.exp(score - top)
                totals = jnp.sum(raised, axis=1, keepdims=True) + jnp.exp(logit - top)
                probs[b, kind, here] = raised.astype(jnp.bfloat16)
                scales[b, kind, here] = jnp.broadcast_to(1.0 / totals, (WINDOW, LANES))
        return carry

    lax.fori_loop(0, blocks, soften, 0)

    half = lax.broadcasted_iota(jnp.int32, (WINDOW, LANES), 1) < HEAD

    def gather(b, carry):
        there = pl.ds(pl.multiple_of(b * WINDOW, WINDOW), span)
        here = pl.ds(pl.multiple_of(b * WINDOW, WINDOW), WINDOW)
        made = [
            jnp.dot(probs[b, kind], values[kind, there], preferred_element_type=jnp.float32)
            * scales[b, kind]
            for kind in range(2)
        ]
        for j in range(2):
            parts = [m[j * WINDOW : (j + 1) * WINDOW] for m in made]
            both = jnp.where(half, parts[j], parts[1 - j])
            out[here, (1 + j) * LANES : (2 + j) * LANES] = both.astype(jnp.bfloat16)
        return carry

    lax.fori_loop(0, blocks, gather, 0)


def attention_call(sink, q, kvp, low, high):
    rows = q.shape[0]
    blocks = rows // WINDOW
    return pl.pallas_call(
        attention_body,
        out_shape=jax.ShapeDtypeStruct((rows, 384), jnp.bfloat16),
        in_specs=[smem] + [vmem] * 4,
        out_specs=vmem,
        scratch_shapes=[
            pltpu.VMEM((2, rows + 2 * WINDOW, LANES), jnp.bfloat16),
            pltpu.VMEM((2, rows + 2 * WINDOW, LANES), jnp.bfloat16),
            pltpu.VMEM((2, blocks, 2 * WINDOW, LANES), jnp.bfloat16),
            pltpu.VMEM((blocks, 2, 2 * WINDOW, 3 * WINDOW), jnp.float32),
            pltpu.VMEM((blocks, 2, 2 * WINDOW, 3 * WINDOW), jnp.bfloat16),
            pltpu.VMEM((blocks, 2, 2 * WINDOW, LANES), jnp.float32),
            pltpu.VMEM((rows + 2 * pool_reach, LANES), jnp.float32),
        ],
        cost_estimate=cost(60 * rows * 4 * 3 * WINDOW * 4, 4 * rows * 256 * 2),
        name="attention",
        compiler_params=limit(20),
    )(sink, q, kvp, low, high)


def order_body(*refs):
    by_x, out = refs[:4], refs[4]
    z, x, _, _ = spot()

    def over_z(i, carry):
        to = around(z, zigzag(i), NZ)
        for j, step in enumerate(X_ORDER):
            here = pl.ds(pl.multiple_of(around(x, step, NX) * LANES, LANES), LANES)
            for k in range(3):
                out[to, k * TILE : (k + 1) * TILE, here] = by_x[j][i, k]
        return carry

    lax.fori_loop(0, 8, over_z, 0)


def order_call(by_x):
    return pl.pallas_call(
        order_body,
        out_shape=jax.ShapeDtypeStruct((8, 3 * TILE, 4 * LANES), jnp.bfloat16),
        in_specs=[vmem] * 4,
        out_specs=vmem,
        cost_estimate=cost(5000000, 6000000),
        name="order",
        compiler_params=limit(10),
    )(*by_x)


def out_body(first, att, weights, mine, theirs, done):
    _, _, y, core = spot()
    columns = weights.shape[2]
    steps = mine.shape[2] // columns

    def over_columns(step, carry):
        total = jnp.dot(att[...], weights[first + step], preferred_element_type=jnp.float32)
        done[...] = total.astype(jnp.bfloat16).reshape(done.shape)
        here = pl.ds(pl.multiple_of(step * columns, columns), columns)
        for r in range(4):
            owner = 2 * around(y, r, NY)
            mine[r, :, here] = done[owner + core]
            theirs[r, :, here] = done[owner + 1 - core]
        return carry

    lax.fori_loop(0, steps, over_columns, 0)


def out_call(att, weights, part, parts):
    rows = att.shape[0]
    share = rows // 8
    columns = 4 * LANES
    steps = 8 // parts
    made = jax.ShapeDtypeStruct((4, share, steps * columns), jnp.bfloat16)
    return pl.pallas_call(
        functools.partial(out_body, part * steps),
        out_shape=(made, made),
        in_specs=[vmem, vmem],
        out_specs=(vmem, vmem),
        scratch_shapes=[pltpu.VMEM((8, share, columns), jnp.bfloat16)],
        cost_estimate=cost(2 * rows * 384 * 512 * steps, 2 * rows * 512 * steps),
        compiler_params=limit(12),
    )(att, weights)


def ring_z(own, far):
    up, down = own, own
    held = [own]
    for _ in range(1, 4):
        up = lax.ppermute(up, "sp", z_moves(1))
        down = lax.ppermute(down, "sp", z_moves(-1))
        held += [up, down]
    return held + [lax.ppermute(up if far == 1 else down, "sp", z_moves(far))]


def ring_x(own, far):
    before = lax.ppermute(own, "sp", x_moves(1))
    after = lax.ppermute(own, "sp", x_moves(-1))
    return [own, before, after, lax.ppermute(before if far == 1 else after, "sp", x_moves(far))]


def plus(*parts):
    total = parts[0].astype(jnp.float32)
    for part in parts[1:]:
        total = total + part.astype(jnp.float32)
    return total.astype(jnp.bfloat16)


def scatter_sum(mine, theirs):
    swapped = lax.ppermute(theirs, "tp", core_moves)
    half = mine.shape[1] // 2
    low = lax.ppermute(plus(mine[2, :half], swapped[2, :half]), "tp", y_moves(1))
    high = lax.ppermute(plus(mine[2, half:], swapped[2, half:]), "tp", y_moves(-1))
    up = jnp.concatenate(
        [plus(mine[1, :half], swapped[1, :half], low), plus(mine[1, half:], swapped[1, half:])]
    )
    down = jnp.concatenate(
        [plus(mine[3, :half], swapped[3, :half]), plus(mine[3, half:], swapped[3, half:], high)]
    )
    return plus(
        mine[0],
        swapped[0],
        lax.ppermute(up, "tp", y_moves(1)),
        lax.ppermute(down, "tp", y_moves(-1)),
    )


def layer(
    tokens,
    norm_gain,
    w_query,
    w_key,
    w_value,
    w_pool,
    query_gain,
    key_gain,
    sink_logit,
    w_out_pool,
    w_out_attn,
):
    rows = tokens.shape[0]
    sp, tp = lax.axis_index("sp"), lax.axis_index("tp")

    before = lax.ppermute(tokens, "tp", y_moves(1))
    after = lax.ppermute(tokens, "tp", y_moves(-1))
    w_block, kvp_block = tile_call(w_query, w_key, w_value, w_pool, w_out_pool, w_out_attn)

    near = [lax.ppermute(kvp_block, "sp", x_moves(-step)) for i, step in enumerate(X_ORDER) if i]
    held = ring_z(w_block, 1)
    by_z = ring_z(jnp.stack([kvp_block] + near), -1)
    farthest = lax.ppermute(jnp.where(tp % 2 == 0, before, after), "tp", split_moves)
    pieces = [tokens, before, after, farthest]
    squares = square_call(pieces)
    squares = (squares, lax.ppermute(squares, "tp", core_moves))
    xs = norm_call(pieces, norm_gain.reshape(8, 1, -1), squares)
    xs = (xs, lax.ppermute(xs, "tp", core_moves))
    q_block, out_block = regroup_call(held)
    by_x = ring_x(q_block, 1)
    out_by_x = ring_x(out_block, -1)

    turns = turn_tables(sp * (rows // GRID_W), 80)
    twice = lambda g: jnp.concatenate([g, g]).reshape(1, LANES)

    kvp, first_rows, last_rows = kvp_call(xs, by_z, twice(key_gain), turns)
    q = q_call(xs, by_x, twice(query_gain), turns)
    count = NZ * NX
    forward = [(i, (i + 1) % count) for i in range(count)]
    backward = [(b, a) for a, b in forward]
    low = lax.ppermute(last_rows, "sp", forward)
    high = lax.ppermute(first_rows, "sp", backward)
    weights = order_call(out_by_x)
    att = attention_call(sink_logit, q, kvp, low, high)
    sums = []
    for part in range(2):
        halves = out_call(att, weights, part, 2)
        sums.append(scatter_sum(*halves))
    return jnp.concatenate([s.reshape(rows // 8, -1) for s in sums], axis=1)


def solution(mesh):
    placed = (
        P("sp", "tp"),
        P(),
        P("sp", "tp"),
        P("sp", "tp"),
        P("sp", "tp"),
        P("sp", "tp"),
        P(),
        P(),
        P("tp"),
        P("tp", "sp"),
        P("tp", "sp"),
    )
    return jax.shard_map(
        layer, mesh=mesh, in_specs=placed, out_specs=P(("sp", "tp"), None), check_vma=False
    )
```

```python
import functools

import jax
import jax.numpy as jnp
import numpy as np
from jax import lax
from jax.experimental import pallas as pl
from jax.experimental.pallas import tpu as pltpu
from jax.sharding import PartitionSpec as P

HEAD = 64
WINDOW = 128
GRID_W = 64
NX, NZ, NY = 4, 8, 4
TILE = 128
LANES = 128
ROWS = 256

eps = 1e-06
rope_base = 10000.0
neg_big = -1e30
pool_reach = 8


Y_ORDER = (0, -1, 1, 2)
X_ORDER = (0, -1, 1, 2)
Z_ORDER = (0, -1, 1, -2, 2, -3, 3, 4)
EARLY = 4


def spot():
    sp, tp = lax.axis_index("sp"), lax.axis_index("tp")
    return lax.div(sp, NX), lax.rem(sp, NX), lax.div(tp, 2), lax.rem(tp, 2)


def around(place, offset, count):
    return lax.rem(place + (offset + count), count)


def z_moves(step):
    return [(z * NX + x, (z + step) % NZ * NX + x) for z in range(NZ) for x in range(NX)]


def x_moves(step):
    return [(z * NX + x, z * NX + (x + step) % NX) for z in range(NZ) for x in range(NX)]


def y_moves(step):
    return [(y * 2 + c, (y + step) % NY * 2 + c) for y in range(NY) for c in range(2)]


core_moves = [(t, t ^ 1) for t in range(2 * NY)]
split_moves = [
    (2 * y + c, (y + 1 - 2 * c) % NY * 2 + c) for y in range(NY) for c in range(2)
]


def cost(flops, nbytes):
    return pl.CostEstimate(flops=flops, bytes_accessed=nbytes, transcendentals=0)


def whole_spec(a):
    return pl.BlockSpec(a.shape, lambda i: (0,) * a.ndim)


def limit(mebibytes):
    return pltpu.CompilerParams(vmem_limit_bytes=mebibytes << 20)


def zigzag(i):
    return lax.select(lax.rem(i, 2) == 1, -lax.div(i + 1, 2), lax.div(i, 2))


vmem = pl.BlockSpec(memory_space=pltpu.VMEM)
smem = pl.BlockSpec(memory_space=pltpu.SMEM)


def tile_body(wq, wk, wv, wp, wop, woa, first, second):
    first[0] = wop[...]
    first[1] = woa[:TILE]
    first[2] = woa[TILE:]
    first[3] = wq[:, :LANES]
    first[4] = wq[:, LANES:]
    second[0] = wk[...]
    second[1] = wv[...]
    second[2] = wp[...]


def tile_call(*weights):
    return pl.pallas_call(
        tile_body,
        out_shape=(
            jax.ShapeDtypeStruct((5, TILE, LANES), jnp.bfloat16),
            jax.ShapeDtypeStruct((3, TILE, LANES), jnp.bfloat16),
        ),
        in_specs=[vmem] * 6,
        out_specs=(vmem, vmem),
        name="tiles",
        cost_estimate=cost(1000000, 500000),
    )(*weights)


def pack_body(*refs):
    for i, block in enumerate(refs[:-1]):
        refs[-1][i] = block[...]


def pack_call(blocks):
    return pl.pallas_call(
        pack_body,
        out_shape=jax.ShapeDtypeStruct((len(blocks),) + blocks[0].shape, blocks[0].dtype),
        in_specs=[vmem] * len(blocks),
        out_specs=vmem,
        name="pack",
        cost_estimate=cost(1000000, 2000000),
        compiler_params=limit(4),
    )(*blocks)


def token_places(y, core):
    return [2 * around(y, step, NY) + core for step in Y_ORDER]


def square_body(*refs):
    pieces, squares = refs[:4], refs[4]

    def chunk(i, carry):
        here = pl.ds(pl.multiple_of(i * 16, 16), 16)
        total = None
        for piece in pieces:
            wide = piece[here].astype(jnp.float32)
            square = wide * wide
            for k in range(0, square.shape[1], LANES):
                part = square[:, k : k + LANES]
                total = part if total is None else total + part
        squares[here] = total
        return carry

    lax.fori_loop(0, squares.shape[0] // 16, chunk, 0, unroll=2)


def square_call(pieces):
    rows, width = pieces[0].shape
    return pl.pallas_call(
        square_body,
        out_shape=jax.ShapeDtypeStruct((rows, LANES), jnp.float32),
        in_specs=[vmem] * 4,
        out_specs=vmem,
        cost_estimate=cost(10 * rows * 4 * width, 2 * rows * 4 * width),
        name="square",
        compiler_params=limit(6),
    )(*pieces)


def norm_body(*refs):
    pieces, gain, own_squares, other_squares, out = refs[:4], *refs[4:]
    _, _, y, core = spot()
    gains = [gain[place] for place in token_places(y, core)]

    def chunk(i, carry):
        here = pl.ds(pl.multiple_of(i * 32, 32), 32)
        square = jnp.sum(own_squares[here] + other_squares[here], axis=1, keepdims=True)
        scale = lax.rsqrt(square / (8.0 * 512.0) + eps)
        for p, piece in enumerate(pieces):
            wide = piece[here].astype(jnp.float32)
            out[p, here] = (wide * scale * gains[p]).astype(jnp.bfloat16)
        return carry

    lax.fori_loop(0, out.shape[1] // 32, chunk, 0, unroll=2)


def norm_call(pieces, gain, squares):
    rows, width = pieces[0].shape
    return pl.pallas_call(
        norm_body,
        out_shape=jax.ShapeDtypeStruct((4, rows, width), jnp.bfloat16),
        in_specs=[vmem] * 7,
        out_specs=vmem,
        cost_estimate=cost(20 * rows * 4 * width, 2 * rows * 8 * width),
        name="norm",
        compiler_params=limit(10),
    )(*pieces, gain, *squares)


def turn_tables(first_row, size):
    within = np.arange(LANES) % HEAD
    freqs = (1.0 / np.float32(rope_base) ** (np.arange(16, dtype=np.float32) * np.float32(2.0 / 32))).astype(np.float32)
    freq = jnp.asarray(freqs[within % 16])[None]
    row_lane = jnp.asarray(within < 32)[None]
    sign = jnp.asarray(np.where(within % 32 < 16, -1.0, 1.0).astype(np.float32))[None]
    at = jnp.arange(size, dtype=jnp.int32)[:, None]
    place = jnp.where(at < GRID_W, at, first_row + at - GRID_W).astype(jnp.float32)
    angle = place * freq
    mine = (at >= GRID_W) == row_lane
    return jnp.stack([jnp.where(mine, jnp.cos(angle), 0.0), jnp.where(mine, jnp.sin(angle) * sign, 0.0)])


def headed(part, gain, cosine, sine):
    lane = lax.broadcasted_iota(jnp.int32, part.shape, 1)
    left = lane < HEAD
    square = part * part
    low = jnp.sum(jnp.where(left, square, 0.0), axis=1, keepdims=True)
    high = jnp.sum(jnp.where(left, 0.0, square), axis=1, keepdims=True)
    scale = jnp.where(left, lax.rsqrt(low / HEAD + eps), lax.rsqrt(high / HEAD + eps))
    scaled = part * scale * gain
    turned = jnp.where(
        lane % 32 < 16, pltpu.roll(scaled, LANES - 16, 1), pltpu.roll(scaled, 16, 1)
    )
    return (scaled * cosine + turned * sine).astype(jnp.bfloat16)


def multiply(own_x, other_x, weights, total):
    _, _, y, core = spot()
    pieces = [
        (part, p, place)
        for part, c in ((own_x, core), (other_x, 1 - core))
        for p, place in enumerate(token_places(y, c))
    ]

    def over_blocks(step, carry):
        block = pl.ds(pl.multiple_of(step * ROWS, ROWS), ROWS)
        made = None
        for part, p, place in pieces:
            one = jnp.dot(part[p, block], weights[place], preferred_element_type=jnp.float32)
            made = one if made is None else made + one
        total[block] = made
        return carry

    lax.fori_loop(0, total.shape[0] // ROWS, over_blocks, 0)


SPAN = 2 * GRID_W


def turned_rows(turns, g):
    rows = [pl.ds(GRID_W + g * (SPAN // GRID_W) + i, 1) for i in range(SPAN // GRID_W)]
    return [
        jnp.concatenate([turns[t, :GRID_W] + turns[t, row] for row in rows], axis=0)
        for t in range(2)
    ]


def kvp_body(own_x, other_x, *refs):
    by_z = refs[:8]
    gain, turns, out, first_out, last_out, weights, total = refs[8:]
    z, x, _, _ = spot()
    z_at = [around(z, offset, NZ) for offset in Z_ORDER]
    rows = out.shape[0]

    def over_x(j, carry):
        here = pl.ds(pl.multiple_of(around(x, zigzag(j), NX) * TILE, TILE), TILE)
        for i in range(8):
            for k in range(3):
                weights[z_at[i], here, k * LANES : (k + 1) * LANES] = by_z[i][j, k]
        return carry

    lax.fori_loop(0, 4, over_x, 0)
    multiply(own_x, other_x, weights, total)

    def over_rows(g, carry):
        here = pl.ds(pl.multiple_of(g * SPAN, SPAN), SPAN)
        cosine, sine = turned_rows(turns, g)
        out[here, :LANES] = headed(total[here, :LANES], gain[...], cosine, sine)
        out[here, LANES:] = total[here, LANES:].astype(jnp.bfloat16)
        return carry

    lax.fori_loop(0, rows // SPAN, over_rows, 0)
    first_out[...] = out[:WINDOW]
    last_out[...] = out[rows - WINDOW :]


def q_body(own_x, other_x, *refs):
    early, late = refs[:8], refs[8:16]
    gain, turns, out, weights, total = refs[16:]
    z, x, _, _ = spot()
    x_at = [around(x, offset, NX) for offset in X_ORDER]

    def over_z(pieces, first, i, carry):
        to = around(z, zigzag(i), NZ)
        for j in range(4):
            here = pl.ds(pl.multiple_of(x_at[j] * TILE, TILE), TILE)
            for k in range(2):
                weights[to, here, k * LANES : (k + 1) * LANES] = pieces[2 * j + k][i - first]
        return carry

    lax.fori_loop(0, EARLY, functools.partial(over_z, early, 0), 0)
    lax.fori_loop(EARLY, 8, functools.partial(over_z, late, EARLY), 0)
    multiply(own_x, other_x, weights, total)

    def over_rows(g, carry):
        here = pl.ds(pl.multiple_of(g * SPAN, SPAN), SPAN)
        cosine, sine = turned_rows(turns, g)
        for j in range(2):
            lanes = slice(j * LANES, (j + 1) * LANES)
            out[here, lanes] = headed(total[here, lanes], gain[...], cosine, sine)
        return carry

    lax.fori_loop(0, out.shape[0] // SPAN, over_rows, 0)


def kvp_call(xs, by_z, gain, turns):
    rows = xs[0].shape[1]
    edge = jax.ShapeDtypeStruct((WINDOW, 384), jnp.bfloat16)
    return pl.pallas_call(
        kvp_body,
        out_shape=(jax.ShapeDtypeStruct((rows, 384), jnp.bfloat16), edge, edge),
        in_specs=[vmem] * 12,
        out_specs=(vmem,) * 3,
        scratch_shapes=[
            pltpu.VMEM((8, 512, 384), jnp.bfloat16),
            pltpu.VMEM((rows, 384), jnp.float32),
        ],
        cost_estimate=cost(2 * rows * 4096 * 384, 2 * rows * 4096 + 2 * 4096 * 384),
        name="kvp",
        compiler_params=limit(18),
    )(*xs, *by_z, gain, turns)


def q_call(xs, by_x, gain, turns):
    rows = xs[0].shape[1]
    return pl.pallas_call(
        q_body,
        out_shape=jax.ShapeDtypeStruct((rows, 256), jnp.bfloat16),
        grid=(1,),
        in_specs=[whole_spec(a) for a in xs]
        + [
            pl.BlockSpec((a.shape[0], None, TILE, LANES), lambda i, k=k: (0, 3 + k, 0, 0))
            for a in by_x
            for k in range(2)
        ]
        + [whole_spec(gain), whole_spec(turns)],
        out_specs=pl.BlockSpec((rows, 256), lambda i: (0, 0)),
        scratch_shapes=[
            pltpu.VMEM((8, 512, 256), jnp.bfloat16),
            pltpu.VMEM((rows, 256), jnp.float32),
        ],
        cost_estimate=cost(2 * rows * 4096 * 256, 2 * rows * 4096 + 2 * 4096 * 256),
        name="q",
        compiler_params=limit(16),
    )(*xs, *(a for a in by_x for _ in range(2)), gain, turns)


def attention_body(
    sink, q, kvp, low, high, out, keys, values, queries, scores, probs, scales, band
):
    rows = q.shape[0]
    blocks = rows // WINDOW
    _, _, level, _ = spot()
    start = lax.axis_index("sp") * rows
    seq = NZ * NX * rows
    span = 3 * WINDOW

    def fill(part, here, there):
        for half, held in ((0, keys), (1, values)):
            block = part[here, half * LANES : (half + 1) * LANES]
            held[0, there] = block
            held[1, there] = jnp.concatenate([block[:, HEAD:], block[:, :HEAD]], axis=1)

    left = lax.broadcasted_iota(jnp.int32, (WINDOW, LANES), 1) < HEAD

    def prepare(b, carry):
        here = pl.ds(pl.multiple_of(b * WINDOW, WINDOW), WINDOW)
        fill(kvp, here, pl.ds(pl.multiple_of((b + 1) * WINDOW, WINDOW), WINDOW))
        for j in range(2):
            pair = q[here, j * LANES : (j + 1) * LANES] * HEAD ** (-0.5)
            for e in range(2):
                alone = jnp.where(left if e == 0 else ~left, pair, 0).astype(jnp.bfloat16)
                queries[int(e != j), b, j * WINDOW : (j + 1) * WINDOW] = alone
        return carry

    lax.fori_loop(0, blocks, prepare, 0)
    fill(low, slice(0, WINDOW), slice(0, WINDOW))
    fill(high, slice(0, WINDOW), slice(WINDOW + rows, 2 * WINDOW + rows))

    pool_low = low[WINDOW - 16 :, 2 * LANES :].astype(jnp.float32)[16 - pool_reach :]
    pool_high = high[:16, 2 * LANES :].astype(jnp.float32)[:pool_reach]
    band[:pool_reach] = jnp.where(start > 0, pool_low, 0.0)
    band[pool_reach : pool_reach + rows] = kvp[:, 2 * LANES :].astype(jnp.float32)
    band[pool_reach + rows :] = jnp.where(start + rows < seq, pool_high, 0.0)
    at = lax.broadcasted_iota(jnp.int32, (WINDOW, LANES), 0)
    reach = lax.shift_left(jnp.int32(1), level)

    def pool(b, carry):
        total = band[pl.ds(pl.multiple_of(b * WINDOW, WINDOW), WINDOW + 2 * pool_reach)]
        chosen = None
        for side in range(4):
            width = 2**side
            total = total[:-width] + total[width:]
            part = total[pool_reach - width : pool_reach - width + WINDOW]
            chosen = part if chosen is None else jnp.where(level == side, part, chosen)
        position = start + b * WINDOW + at
        first = jnp.maximum(position - reach, 0)
        last = jnp.minimum(position + reach - 1, seq - 1)
        counted = (last - first + 1).astype(jnp.float32)
        here = pl.ds(pl.multiple_of(b * WINDOW, WINDOW), WINDOW)
        out[here, :LANES] = (chosen / counted).astype(jnp.bfloat16)
        return carry

    lax.fori_loop(0, blocks, pool, 0)

    def score(b, carry):
        there = pl.ds(pl.multiple_of(b * WINDOW, WINDOW), span)
        for kind in range(2):
            scores[b, kind] = lax.dot_general(
                queries[kind, b],
                keys[kind, there],
                (((1,), (1,)), ((), ())),
                preferred_element_type=jnp.float32,
            )
        return carry

    lax.fori_loop(0, blocks, score, 0, unroll=2)

    ahead = lax.broadcasted_iota(jnp.int32, (WINDOW, span), 1) - lax.broadcasted_iota(
        jnp.int32, (WINDOW, span), 0
    )
    near = (ahead >= 0) & (ahead <= 2 * WINDOW)
    key_at = lax.broadcasted_iota(jnp.int32, (WINDOW, span), 1)

    def soften(b, carry):
        origin = start + (b - 1) * WINDOW
        inside = near & (key_at >= -origin) & (key_at < seq - origin)
        for kind in range(2):
            for j in range(2):
                logit = sink[2 * j + (j if kind == 0 else 1 - j)]
                here = pl.ds(j * WINDOW, WINDOW)
                score = jnp.where(inside, scores[b, kind, here], neg_big)
                top = jnp.maximum(jnp.max(score, axis=1, keepdims=True), logit)
                raised = jnp.exp(score - top)
                totals = jnp.sum(raised, axis=1, keepdims=True) + jnp.exp(logit - top)
                probs[b, kind, here] = raised.astype(jnp.bfloat16)
                scales[b, kind, here] = jnp.broadcast_to(1.0 / totals, (WINDOW, LANES))
        return carry

    lax.fori_loop(0, blocks, soften, 0)

    half = lax.broadcasted_iota(jnp.int32, (WINDOW, LANES), 1) < HEAD

    def gather(b, carry):
        there = pl.ds(pl.multiple_of(b * WINDOW, WINDOW), span)
        here = pl.ds(pl.multiple_of(b * WINDOW, WINDOW), WINDOW)
        made = [
            jnp.dot(probs[b, kind], values[kind, there], preferred_element_type=jnp.float32)
            * scales[b, kind]
            for kind in range(2)
        ]
        for j in range(2):
            parts = [m[j * WINDOW : (j + 1) * WINDOW] for m in made]
            both = jnp.where(half, parts[j], parts[1 - j])
            out[here, (1 + j) * LANES : (2 + j) * LANES] = both.astype(jnp.bfloat16)
        return carry

    lax.fori_loop(0, blocks, gather, 0)


def attention_call(sink, q, kvp, low, high):
    rows = q.shape[0]
    blocks = rows // WINDOW
    return pl.pallas_call(
        attention_body,
        out_shape=jax.ShapeDtypeStruct((rows, 384), jnp.bfloat16),
        in_specs=[smem] + [vmem] * 4,
        out_specs=vmem,
        scratch_shapes=[
            pltpu.VMEM((2, rows + 2 * WINDOW, LANES), jnp.bfloat16),
            pltpu.VMEM((2, rows + 2 * WINDOW, LANES), jnp.bfloat16),
            pltpu.VMEM((2, blocks, 2 * WINDOW, LANES), jnp.bfloat16),
            pltpu.VMEM((blocks, 2, 2 * WINDOW, 3 * WINDOW), jnp.float32),
            pltpu.VMEM((blocks, 2, 2 * WINDOW, 3 * WINDOW), jnp.bfloat16),
            pltpu.VMEM((blocks, 2, 2 * WINDOW, LANES), jnp.float32),
            pltpu.VMEM((rows + 2 * pool_reach, LANES), jnp.float32),
        ],
        cost_estimate=cost(60 * rows * 4 * 3 * WINDOW * 4, 4 * rows * 256 * 2),
        name="attention",
        compiler_params=limit(20),
    )(sink, q, kvp, low, high)


def order_body(*refs):
    early, late, out = refs[:4], refs[4:8], refs[8]
    z, x, _, _ = spot()

    def over_z(pieces, first, i, carry):
        to = around(z, zigzag(i), NZ)
        for j, step in enumerate(X_ORDER):
            here = pl.ds(pl.multiple_of(around(x, step, NX) * LANES, LANES), LANES)
            for k in range(3):
                out[to, k * TILE : (k + 1) * TILE, here] = pieces[j][i - first, k]
        return carry

    lax.fori_loop(0, EARLY, functools.partial(over_z, early, 0), 0)
    lax.fori_loop(EARLY, 8, functools.partial(over_z, late, EARLY), 0)


def order_call(by_x):
    return pl.pallas_call(
        order_body,
        out_shape=jax.ShapeDtypeStruct((8, 3 * TILE, 4 * LANES), jnp.bfloat16),
        grid=(1,),
        in_specs=[pl.BlockSpec((a.shape[0], 3, TILE, LANES), lambda i: (0, 0, 0, 0)) for a in by_x],
        out_specs=pl.BlockSpec((8, 3 * TILE, 4 * LANES), lambda i: (0, 0, 0)),
        cost_estimate=cost(5000000, 6000000),
        name="order",
        compiler_params=limit(14),
    )(*by_x)


def out_body(first, att, weights, mine, theirs, done):
    _, _, y, core = spot()
    columns = weights.shape[2]
    steps = mine.shape[2] // columns

    def over_columns(step, carry):
        total = jnp.dot(att[...], weights[first + step], preferred_element_type=jnp.float32)
        done[...] = total.astype(jnp.bfloat16).reshape(done.shape)
        here = pl.ds(pl.multiple_of(step * columns, columns), columns)
        for r in range(4):
            owner = 2 * around(y, r, NY)
            mine[r, :, here] = done[owner + core]
            theirs[r, :, here] = done[owner + 1 - core]
        return carry

    lax.fori_loop(0, steps, over_columns, 0)


def out_call(att, weights, part, parts):
    rows = att.shape[0]
    share = rows // 8
    columns = 4 * LANES
    steps = 8 // parts
    made = jax.ShapeDtypeStruct((4, share, steps * columns), jnp.bfloat16)
    return pl.pallas_call(
        functools.partial(out_body, part * steps),
        out_shape=(made, made),
        in_specs=[vmem, vmem],
        out_specs=(vmem, vmem),
        scratch_shapes=[pltpu.VMEM((8, share, columns), jnp.bfloat16)],
        cost_estimate=cost(2 * rows * 384 * 512 * steps, 2 * rows * 512 * steps),
        compiler_params=limit(12),
    )(att, weights)


def ring_z(own, far):
    up, down = own, own
    held = [own]
    for _ in range(1, 4):
        up = lax.ppermute(up, "sp", z_moves(1))
        down = lax.ppermute(down, "sp", z_moves(-1))
        held += [up, down]
    return held + [lax.ppermute(up if far == 1 else down, "sp", z_moves(far))]


def ring_x(own, far):
    before = lax.ppermute(own, "sp", x_moves(1))
    after = lax.ppermute(own, "sp", x_moves(-1))
    return [own, before, after, lax.ppermute(before if far == 1 else after, "sp", x_moves(far))]


def plus(*parts):
    total = parts[0].astype(jnp.float32)
    for part in parts[1:]:
        total = total + part.astype(jnp.float32)
    return total.astype(jnp.bfloat16)


def scatter_sum(mine, theirs):
    swapped = lax.ppermute(theirs, "tp", core_moves)
    half = mine.shape[1] // 2
    low = lax.ppermute(plus(mine[2, :half], swapped[2, :half]), "tp", y_moves(1))
    high = lax.ppermute(plus(mine[2, half:], swapped[2, half:]), "tp", y_moves(-1))
    up = plus(mine[1], swapped[1], jnp.pad(low, ((0, half), (0, 0))))
    down = plus(mine[3], swapped[3], jnp.pad(high, ((half, 0), (0, 0))))
    return plus(
        mine[0],
        swapped[0],
        lax.ppermute(up, "tp", y_moves(1)),
        lax.ppermute(down, "tp", y_moves(-1)),
    )


def layer(
    tokens,
    norm_gain,
    w_query,
    w_key,
    w_value,
    w_pool,
    query_gain,
    key_gain,
    sink_logit,
    w_out_pool,
    w_out_attn,
):
    rows = tokens.shape[0]
    sp, tp = lax.axis_index("sp"), lax.axis_index("tp")

    before = lax.ppermute(tokens, "tp", y_moves(1))
    after = lax.ppermute(tokens, "tp", y_moves(-1))
    w_block, kvp_block = tile_call(w_query, w_key, w_value, w_pool, w_out_pool, w_out_attn)

    near = [lax.ppermute(kvp_block, "sp", x_moves(-step)) for i, step in enumerate(X_ORDER) if i]
    held = ring_z(w_block, 1)
    by_z = ring_z(jnp.stack([kvp_block] + near), -1)
    farthest = lax.ppermute(jnp.where(tp % 2 == 0, before, after), "tp", split_moves)
    pieces = [tokens, before, after, farthest]
    squares = square_call(pieces)
    squares = (squares, lax.ppermute(squares, "tp", core_moves))
    xs = norm_call(pieces, norm_gain.reshape(8, 1, -1), squares)
    xs = (xs, lax.ppermute(xs, "tp", core_moves))
    by_x = ring_x(pack_call(held[:EARLY]), 1) + ring_x(pack_call(held[EARLY:]), -1)

    turns = turn_tables(sp * (rows // GRID_W), 80)
    twice = lambda g: jnp.concatenate([g, g]).reshape(1, LANES)

    kvp, first_rows, last_rows = kvp_call(xs, by_z, twice(key_gain), turns)
    q = q_call(xs, by_x, twice(query_gain), turns)
    count = NZ * NX
    forward = [(i, (i + 1) % count) for i in range(count)]
    backward = [(b, a) for a, b in forward]
    low = lax.ppermute(last_rows, "sp", forward)
    high = lax.ppermute(first_rows, "sp", backward)
    weights = order_call(by_x)
    att = attention_call(sink_logit, q, kvp, low, high)
    sums = []
    for part in range(2):
        halves = out_call(att, weights, part, 2)
        sums.append(scatter_sum(*halves))
    return jnp.concatenate([s.reshape(rows // 8, -1) for s in sums], axis=1)


def solution(mesh):
    placed = (
        P("sp", "tp"),
        P(),
        P("sp", "tp"),
        P("sp", "tp"),
        P("sp", "tp"),
        P("sp", "tp"),
        P(),
        P(),
        P("tp"),
        P("tp", "sp"),
        P("tp", "sp"),
    )
    return jax.shard_map(
        layer, mesh=mesh, in_specs=placed, out_specs=P(("sp", "tp"), None), check_vma=False
    )
```
